32 devices in a mesh: sp: 4 (over y, x), tp: 8 (over z, core).
Axes of the slice: x: 2, y: 2, z: 4, core: 2. Of those that a mesh axis runs over, the one named last changes fastest.
Arguments:
- stream: bfloat16 [8, 1536, 2048], P('tp', 'sp'), may hold values from -80 to 80
- norm_gain: float32 [2048], replicated, may hold values from 0.1 to 1.9
- w_lin: bfloat16 [1024, 2048], P('tp'), may hold values from -0.125 to 0.125
- w_gate: bfloat16 [1024, 2048], P('tp'), may hold values from -0.125 to 0.125
- conv_taps: bfloat16 [31, 1024], replicated, may hold values from -3 to 3
- conv_bias: float32 [1024], replicated, may hold values from -3 to 3
- ln_gain: float32 [1024], replicated, may hold values from 0.1 to 1.9
- ln_shift: float32 [1024], replicated, may hold values from -3 to 3
- w_proj: bfloat16 [1024, 2048], P('tp'), may hold values from -0.1875 to 0.1875
Outputs:
- result_stream: bfloat16 [8, 1536, 2048], P('tp', 'sp')
The draws below stay inside these ranges and needn't reach their ends.
All inputs are finite; a program needn't handle non-finite values.
Results may differ from the reference program's by a relative error of at most 0.0024.
Values may be sent and summed in bfloat16 or wider, within the bound.
A program may use at most 64 MiB of HBM per device.

```python
import jax
import jax.numpy as jnp
from jax import lax

D = 2048
CC = 1024
KW = 31
SEQ_LEN = 1536
SEQS = 8


def draw_stream(key, part):
    k_base, k_cols, k_rows = jax.random.split(jax.random.fold_in(key, 11), 3)
    cols = jnp.arange(D, dtype=jnp.float32) / D
    col_scale = jnp.exp(jnp.log(4.0) * cols) * jnp.exp(jax.random.uniform(k_cols, (D,), jnp.float32, -0.35, 0.35))
    row_scale = jnp.exp(jax.random.uniform(k_rows, (SEQS, SEQ_LEN, 1), jnp.float32, 0.0, jnp.log(10.0))) / 3.0
    base = jnp.clip(jax.random.normal(k_base, (SEQS, SEQ_LEN, D), jnp.float32), -4.0, 4.0)
    return (base * row_scale * col_scale).astype(jnp.bfloat16)


def draw_conv_taps(key, part):
    k_base, k_cols = jax.random.split(jax.random.fold_in(key, 23), 2)
    cols = jnp.arange(CC, dtype=jnp.float32) / CC
    col_scale = jnp.exp(jnp.log(3.0) * cols) * jnp.exp(jax.random.uniform(k_cols, (1, CC), jnp.float32, -0.35, 0.35))
    base = jnp.clip(jax.random.normal(k_base, (KW, CC), jnp.float32), -3.5, 3.5)
    return (base * col_scale * KW ** (-0.5)).astype(jnp.bfloat16)


def level_of(stream_key, dims, pieces, smallest, top_value):
    loudness = 1.0
    for dim, shards_of in pieces:
        draws = jax.random.uniform(jax.random.fold_in(jax.random.fold_in(stream_key, 6), dim), (shards_of,), jnp.float32, smallest / len(pieces), top_value / len(pieces))
        loudness = loudness * jnp.repeat(jnp.exp(draws), dims[dim] // shards_of).reshape((-1,) + (1,) * (len(dims) - 1 - dim))
    return loudness


def gaussian(key, shape, deviation, reach, cuts=(), kind=jnp.bfloat16):
    drawn = deviation * jax.random.normal(key, shape, jnp.float32)
    if cuts:
        drawn = drawn * level_of(key, shape, cuts, -0.22, 0.18)
    return jnp.clip(drawn, -reach, reach).astype(kind)


def setup_inputs(seed: int = 0) -> dict:
    seeds = jax.random.split(jax.random.key(seed), 10)
    return {
        "stream": draw_stream(jax.random.fold_in(seeds[9], 71), 0),
        "norm_gain": jnp.clip(1.0 + 0.18 * jax.random.normal(seeds[1], (D,), jnp.float32), 0.1, 1.9),
        "w_lin": gaussian(seeds[2], (CC, D), D ** -0.5, 0.125, ((0, 8),)),
        "w_gate": gaussian(seeds[3], (CC, D), D ** -0.5, 0.125, ((0, 8),)),
        "conv_taps": draw_conv_taps(jax.random.fold_in(seeds[9], 71), 0),
        "conv_bias": gaussian(seeds[5], (CC,), 0.5, 3.0, (), jnp.float32),
        "ln_gain": jnp.clip(1.0 + 0.18 * jax.random.normal(seeds[6], (CC,), jnp.float32), 0.1, 1.9),
        "ln_shift": gaussian(seeds[7], (CC,), 0.5, 3.0, (), jnp.float32),
        "w_proj": gaussian(seeds[8], (CC, D), CC ** -0.5, 0.1875, ((0, 8),)),
    }


EPS = 1e-06

def rms_rows(rows, gain):
    full = rows.astype(jnp.float32)
    scale = lax.rsqrt(lax.optimization_barrier(jnp.mean(full * full, axis=1, keepdims=True)) + EPS)
    return (full * scale * gain.astype(jnp.float32)).astype(jnp.bfloat16)

def project_rows(normed, weight):
    return lax.dot_general(normed, weight, (((1,), (1,)), ((), ())), preferred_element_type=jnp.float32)

def reference(stream, norm_gain, w_lin, w_gate, conv_taps, conv_bias, ln_gain, ln_shift, w_proj):
    taps_full = conv_taps.astype(jnp.float32)

    def one_sequence(current):
        normed = rms_rows(current, norm_gain)
        linear = project_rows(normed, w_lin)
        gating = project_rows(normed, w_gate)
        mixed = (linear * jax.nn.sigmoid(gating)).astype(jnp.bfloat16)
        length = current.shape[0]
        padded = jnp.pad(mixed.astype(jnp.float32), ((KW - 1, 0), (0, 0)))
        conv = jnp.zeros((length, mixed.shape[1]), jnp.float32)
        for tap in range(KW):
            conv = conv + taps_full[tap] * padded[tap:tap + length]
        conv = conv + conv_bias
        mean = lax.optimization_barrier(jnp.mean(conv, axis=1, keepdims=True))
        meansq = lax.optimization_barrier(jnp.mean(conv * conv, axis=1, keepdims=True))
        var = meansq - mean * mean
        activated = jax.nn.silu((conv - mean) * lax.rsqrt(var + EPS) * ln_gain + ln_shift).astype(jnp.bfloat16)
        projected = jnp.dot(activated, w_proj, preferred_element_type=jnp.float32)
        return (current.astype(jnp.float32) + projected).astype(jnp.bfloat16)
    return lax.map(one_sequence, stream)
```

```python
import functools

import jax
import jax.numpy as jnp
from jax import lax
from jax.experimental import pallas as pl
from jax.experimental.pallas import tpu as pltpu
from jax.sharding import PartitionSpec as P

EPS = 1e-06
HALO = 32
F32 = jnp.float32
BF16 = jnp.bfloat16
MESH = pl.DeviceIdType.MESH


def kernel(
    nsp, nz, kw,
    x_ref, gain_ref, wl_ref, wg_ref, wp_ref, taps_ref, bias_ref, lng_ref, lnb_ref,
    out_ref,
    held, xh, normed, mix, conv, act, taps,
    local_sem, halo_sem, z_recv, x_recv, y_recv, d_recv, up_send, dn_send, x_send, y_send, d_send,
):
    rows, width = x_ref.shape
    block = held.shape[2]
    shard = block // 2
    lanes = min(128, block)
    strips = block // lanes
    quarter = width // 4
    half = quarter // 2
    p, tp = lax.axis_index("sp"), lax.axis_index("tp")
    z, c = tp // 2, tp % 2
    q = p % 4
    low, high = q % 2, q // 2
    beside = (p + 1 - 2 * low, tp)
    across = (p + 2 - 4 * high, tp)
    twin = (p, z * 2 + 1 - c)
    above = (p, tp + 2)
    below = (p, tp - 2)
    parity = (low + high) % 2
    has_up, has_dn = z < nz - 1, z > 0
    has_next, has_prev = p < nsp - 1, p > 0
    qx, qy, qd = q + 1 - 2 * low, q + 2 - 4 * high, 3 - q

    def cols(start, size):
        return pl.ds(pl.multiple_of(start, 128), size)

    def at(kind, src, core, start, size):
        return held.at[kind, src, pl.ds(pl.multiple_of(core * shard, 16), shard), cols(start, size)]

    def send(piece, ssem, rsem, target):
        return pltpu.make_async_remote_copy(
            src_ref=piece, dst_ref=piece, send_sem=ssem, recv_sem=rsem, device_id=target, device_id_type=MESH
        )

    def z_piece(kind, src, i):
        if kind < 2:
            return at(kind, src, c, q * quarter, quarter)
        return at(kind, src, c, (parity * 2 + i) * quarter, quarter)

    def z_copy(kind, src, i, up):
        return send(
            z_piece(kind, src, i), (up_send if up else dn_send).at[kind, src, i], z_recv.at[kind, src, i],
            above if up else below,
        )

    def z_pieces(kind):
        return 1 if kind < 2 else 2

    def x_copy(kind, src, i, incoming):
        if kind == 2:
            piece = at(2, src, c, ((1 - parity if incoming else parity) * 2) * quarter, quarter)
        elif i == 0:
            piece = at(kind, src, c, (qx if incoming else q) * quarter, quarter)
        else:
            piece = at(kind, src, c, (qd if incoming else qy) * quarter, half)
        return send(piece, x_send.at[kind, src, i], x_recv.at[kind, src, i], beside)

    def y_copy(kind, src, i, incoming):
        if kind == 2:
            piece = at(2, src, c, ((1 - parity if incoming else parity) * 2 + 1) * quarter, quarter)
        elif i == 0:
            piece = at(kind, src, c, (qy if incoming else q) * quarter, quarter)
        else:
            piece = at(kind, src, c, (qd if incoming else qx) * quarter + half, half)
        return send(piece, y_send.at[kind, src, i], y_recv.at[kind, src, i], across)

    def d_copy(kind, src, core):
        return send(at(kind, src, core, 0, width), d_send.at[kind, src], d_recv.at[kind, src], twin)

    def halo_copy():
        return pltpu.make_async_remote_copy(
            src_ref=x_ref.at[pl.ds(rows - HALO, HALO)], dst_ref=xh, send_sem=halo_sem.at[0],
            recv_sem=halo_sem.at[1], device_id=(p + 1, tp), device_id_type=MESH,
        )

    mine = [
        pltpu.make_async_copy(ref, at(kind, z, c, 0, width), local_sem.at[kind])
        for kind, ref in enumerate((wl_ref, wg_ref, wp_ref))
    ]
    for copy in mine:
        copy.start()

    barrier = pltpu.get_barrier_semaphore()
    for target in (beside, across, twin):
        pl.semaphore_signal(barrier, inc=1, device_id=target, device_id_type=MESH)
    for there, target in (
        (has_up, above), (has_dn, below), (has_next, (p + 1, tp)), (has_prev, (p - 1, tp)),
    ):
        @pl.when(there)
        def _():
            pl.semaphore_signal(barrier, inc=1, device_id=target, device_id_type=MESH)

    one = lambda there: jnp.where(there, 1, 0)
    pl.semaphore_wait(barrier, 3 + one(has_up) + one(has_dn) + one(has_next) + one(has_prev))

    def start_own(kind):
        for i in range(z_pieces(kind)):
            @pl.when(has_up)
            def _():
                z_copy(kind, z, i, True).start()

            @pl.when(has_dn)
            def _():
                z_copy(kind, z, i, False).start()

    mine[0].wait()
    start_own(0)
    mine[1].wait()
    start_own(1)
    mine[2].wait()

    @pl.when(has_next)
    def _():
        halo_copy().start()

    for kind in range(3):
        d_copy(kind, z, c).start()

    def each(t, body):
        for sign in (-1, 1):
            src = z + sign * t

            @pl.when((src >= 0) & (src < nz))
            def _():
                body(src, sign)

    def relay(kind):
        def body(src, sign):
            for i in range(z_pieces(kind)):
                z_copy(kind, src, i, True).wait_recv()
                if sign < 0:
                    @pl.when(has_up)
                    def _():
                        z_copy(kind, src, i, True).start()
                else:
                    @pl.when(has_dn)
                    def _():
                        z_copy(kind, src, i, False).start()
                if kind < 2 or i == 0:
                    x_copy(kind, src, 0, False).start()
                if kind < 2 or i == 1:
                    y_copy(kind, src, 0, False).start()

        return body

    def diagonal(kind):
        def body(src, sign):
            x_copy(kind, src, 0, True).wait_recv()
            y_copy(kind, src, 1, False).start()
            y_copy(kind, src, 0, True).wait_recv()
            x_copy(kind, src, 1, False).start()

        return body

    def finish(kind):
        def body(src, sign):
            for i in ((1,) if kind < 2 else (0,)):
                x_copy(kind, src, i, True).wait_recv()
                y_copy(kind, src, i, True).wait_recv()
            d_copy(kind, src, c).start()

        return body

    def norm_into(ref, base, count):
        @pl.loop(0, count // 16)
        def _(r):
            full = ref[pl.ds(pl.multiple_of(r * 16, 16), 16), :].astype(F32)
            scale = lax.rsqrt(jnp.mean(full * full, axis=1, keepdims=True) + EPS)
            normed[pl.ds(pl.multiple_of(base + r * 16, 16), 16), :] = (full * scale * gain_ref[...]).astype(BF16)

    norm_into(x_ref, HALO, rows)
    for i in range(nz):
        taps[i, 0:kw] = taps_ref[:, i * block:(i + 1) * block].astype(F32)
        taps[i, kw:kw + 1] = bias_ref[:, i * block:(i + 1) * block]

    @pl.when(has_prev)
    def _():
        halo_copy().wait_recv()

    @pl.when(jnp.logical_not(has_prev))
    def _():
        xh[...] = jnp.zeros_like(xh)

    norm_into(xh, 0, HALO)

    tile = 64
    lead = HALO - (kw - 1)
    nt = (((1,), (1,)), ((), ()))

    def compute(t):
        def body(side, carry):
            src = z + (2 * side - 1) * t

            valid = (src >= 0) & (src < nz) & ((t > 0) | (side == 0))

            @pl.when(valid)
            def _():
                d_copy(0, src, 1 - c).wait_recv()
                d_copy(1, src, 1 - c).wait_recv()
                linear = lax.dot_general(normed[...], held[0, src], nt, preferred_element_type=F32)
                gating = lax.dot_general(normed[...], held[1, src], nt, preferred_element_type=F32)
                mixed = (linear * jax.nn.sigmoid(gating)).astype(BF16).astype(F32)
                for s in range(strips):
                    mix[s, 0:HALO + rows] = mixed[:, s * lanes:(s + 1) * lanes]

                @pl.loop(0, rows // tile)
                def _(r):
                    base = pl.multiple_of(r * tile, tile)
                    for s in range(strips):
                        lane = slice(s * lanes, (s + 1) * lanes)
                        total = jnp.broadcast_to(taps[src, kw:kw + 1, lane], (tile, lanes))
                        for b in range(8):
                            slab = mix[s, pl.ds(base + b, tile + HALO), :]
                            for a in range(HALO // 8 + 1):
                                tap = 8 * a + b - lead
                                if 0 <= tap < kw:
                                    total = total + taps[src, tap:tap + 1, lane] * slab[8 * a:8 * a + tile]
                        conv[src, pl.ds(base, tile), lane] = total

            return carry

        lax.fori_loop(0, 2, body, 0)

    @pl.loop(1, nz)
    def _(t):
        each(t, relay(0))
        each(t, relay(1))

        @pl.when(t == nz - 1)
        def _():
            start_own(2)

        each(t, diagonal(0))
        compute(t - 1)
        each(t, diagonal(1))
        each(t, finish(0))
        each(t, finish(1))

    each(1, relay(2))
    compute(nz - 1)

    @pl.loop(2, nz - 1)
    def _(t):
        each(t, relay(2))

    channels = nz * block

    @pl.loop(0, rows // 16)
    def _(r):
        here = pl.ds(pl.multiple_of(r * 16, 16), 16)
        parts = [conv[i, here, :] for i in range(nz)]
        mean = sum(jnp.sum(v, axis=1, keepdims=True) for v in parts) / channels
        meansq = sum(jnp.sum(v * v, axis=1, keepdims=True) for v in parts) / channels
        scale = lax.rsqrt(meansq - mean * mean + EPS)
        for i, v in enumerate(parts):
            lane = slice(i * block, (i + 1) * block)
            u = (v - mean) * scale * lng_ref[:, lane] + lnb_ref[:, lane]
            act[i, here, :] = (u * jax.nn.sigmoid(u)).astype(BF16)

    if nz > 2:
        each(nz - 1, relay(2))

    @pl.loop(1, nz)
    def _(t):
        each(t, finish(2))

    @pl.loop(0, nz)
    def _(src):
        d_copy(2, src, 1 - c).wait_recv()

    @pl.loop(0, 4)
    def _(n):
        here = cols(n * quarter, quarter)
        total = x_ref[:, here].astype(F32)
        for i in range(nz):
            total = total + jnp.dot(act[i], held[2, i, :, here], preferred_element_type=F32)
        out_ref[:, here] = total.astype(BF16)

    @pl.when(has_next)
    def _():
        halo_copy().wait_send()

    for kind in range(3):
        @pl.loop(0, nz)
        def _(src):
            d_copy(kind, src, c).wait_send()

            @pl.when(src != z)
            def _():
                for i in range(2 if kind < 2 else 1):
                    x_copy(kind, src, i, False).wait_send()
                    y_copy(kind, src, i, False).wait_send()

            for i in range(z_pieces(kind)):
                @pl.when((src <= z) & has_up)
                def _():
                    z_copy(kind, src, i, True).wait_send()

                @pl.when((src >= z) & has_dn)
                def _():
                    z_copy(kind, src, i, False).wait_send()


def local(nsp, ntp, stream, norm_gain, w_lin, w_gate, conv_taps, conv_bias, ln_gain, ln_shift, w_proj):
    _, rows, width = stream.shape
    kw, channels = conv_taps.shape
    nz = ntp // 2
    block = channels // nz
    lanes = min(128, block)
    vmem = pl.BlockSpec(memory_space=pltpu.VMEM)
    anyw = pl.BlockSpec(memory_space=pl.ANY)
    dma = pltpu.SemaphoreType.DMA
    out = pl.pallas_call(
        functools.partial(kernel, nsp, nz, kw),
        out_shape=jax.ShapeDtypeStruct((rows, width), BF16),
        in_specs=[vmem, vmem, anyw, anyw, anyw, vmem, vmem, vmem, vmem],
        out_specs=vmem,
        scratch_shapes=[
            pltpu.VMEM((3, nz, block, width), BF16),
            pltpu.VMEM((HALO, width), BF16),
            pltpu.VMEM((HALO + rows, width), BF16),
            pltpu.VMEM((block // lanes, HALO + rows + 8, lanes), F32),
            pltpu.VMEM((nz, rows, block), F32),
            pltpu.VMEM((nz, rows, block), BF16),
            pltpu.VMEM((nz, kw + 1, block), F32),
            dma((3,)), dma((2,)),
            dma((3, nz, 2)), dma((3, nz, 2)), dma((3, nz, 2)), dma((3, nz)),
            dma((3, nz, 2)), dma((3, nz, 2)), dma((3, nz, 2)), dma((3, nz, 2)), dma((3, nz)),
        ],
        compiler_params=pltpu.CompilerParams(
            collective_id=0, has_side_effects=True, vmem_limit_bytes=56 * 1024 * 1024
        ),
    )(
        stream[0], norm_gain[None], w_lin, w_gate, w_proj, conv_taps,
        conv_bias[None], ln_gain[None], ln_shift[None],
    )
    return out[None]


def solution(mesh):
    placed = (
        P("tp", "sp", None), P(), P("tp", None), P("tp", None), P(), P(), P(), P(), P("tp", None),
    )
    return jax.shard_map(
        functools.partial(local, mesh.shape["sp"], mesh.shape["tp"]),
        mesh=mesh, in_specs=placed, out_specs=P("tp", "sp", None), check_vma=False,
    )
```

```python
import functools

import jax
import jax.numpy as jnp
from jax import lax
from jax.experimental import pallas as pl
from jax.experimental.pallas import tpu as pltpu
from jax.sharding import PartitionSpec as P

EPS = 1e-06
HALO = 32
F32 = jnp.float32
BF16 = jnp.bfloat16
MESH = pl.DeviceIdType.MESH


def kernel(
    nsp, nz, kw,
    x_any, gain_ref, wl_ref, wg_ref, wp_ref, taps_ref, bias_ref, lng_ref, lnb_ref,
    out_any,
    x_ref, out_ref, held, xh, normed, mix, conv, act, taps,
    local_sem, out_sem, halo_sem, z_recv, x_recv, y_recv, d_recv, up_send, dn_send, x_send, y_send, d_send, dp_recv, dp_send,
):
    rows, width = x_ref.shape
    block = held.shape[2]
    shard = block // 2
    lanes = min(128, block)
    strips = block // lanes
    quarter = width // 4
    half = quarter // 2
    p, tp = lax.axis_index("sp"), lax.axis_index("tp")
    z, c = tp // 2, tp % 2
    q = p % 4
    low, high = q % 2, q // 2
    beside = (p + 1 - 2 * low, tp)
    across = (p + 2 - 4 * high, tp)
    twin = (p, z * 2 + 1 - c)
    above = (p, tp + 2)
    below = (p, tp - 2)
    parity = (low + high) % 2
    has_up, has_dn = z < nz - 1, z > 0
    has_next, has_prev = p < nsp - 1, p > 0
    qx, qy, qd = q + 1 - 2 * low, q + 2 - 4 * high, 3 - q

    def cols(start, size):
        return pl.ds(pl.multiple_of(start, 128), size)

    def at(kind, src, core, start, size):
        return held.at[kind, src, pl.ds(pl.multiple_of(core * shard, 16), shard), cols(start, size)]

    def send(piece, ssem, rsem, target):
        return pltpu.make_async_remote_copy(
            src_ref=piece, dst_ref=piece, send_sem=ssem, recv_sem=rsem, device_id=target, device_id_type=MESH
        )

    def final(kind):
        return isinstance(kind, int) and kind == 2

    def z_piece(kind, src, i):
        if not final(kind):
            return at(kind, src, c, q * quarter, quarter)
        return at(kind, src, c, (parity * 2 + i) * quarter, quarter)

    def z_copy(kind, src, i, up):
        return send(
            z_piece(kind, src, i), (up_send if up else dn_send).at[kind, src, i], z_recv.at[kind, src, i],
            above if up else below,
        )

    def z_pieces(kind):
        return 2 if final(kind) else 1

    def x_copy(kind, src, i, incoming):
        if final(kind):
            piece = at(2, src, c, ((1 - parity if incoming else parity) * 2) * quarter, quarter)
        elif i == 0:
            piece = at(kind, src, c, (qx if incoming else q) * quarter, quarter)
        else:
            piece = at(kind, src, c, (qd if incoming else qy) * quarter, half)
        return send(piece, x_send.at[kind, src, i], x_recv.at[kind, src, i], beside)

    def y_copy(kind, src, i, incoming):
        if final(kind):
            piece = at(2, src, c, ((1 - parity if incoming else parity) * 2 + 1) * quarter, quarter)
        elif i == 0:
            piece = at(kind, src, c, (qy if incoming else q) * quarter, quarter)
        else:
            piece = at(kind, src, c, (qd if incoming else qx) * quarter + half, half)
        return send(piece, y_send.at[kind, src, i], y_recv.at[kind, src, i], across)

    def d_copy(kind, src, core):
        return send(at(kind, src, core, 0, width), d_send.at[kind, src], d_recv.at[kind, src], twin)

    def d_piece(kind, src, start, size):
        return send(at(kind, src, c, start, size), d_send.at[kind, src], d_recv.at[kind, src], twin)

    def p_cols(slot):
        return ((parity + slot // 2) % 2 * 2 + slot % 2) * quarter

    def p_copy(src, slot, core):
        return send(at(2, src, core, p_cols(slot), quarter), dp_send.at[src, slot], dp_recv.at[src, slot], twin)

    def halo_copy():
        return pltpu.make_async_remote_copy(
            src_ref=x_ref.at[pl.ds(rows - HALO, HALO)], dst_ref=xh, send_sem=halo_sem.at[0],
            recv_sem=halo_sem.at[1], device_id=(p + 1, tp), device_id_type=MESH,
        )

    mine = [
        pltpu.make_async_copy(ref, at(kind, z, c, 0, width), local_sem.at[kind])
        for kind, ref in enumerate((wl_ref, wg_ref, wp_ref))
    ]
    stream_in = pltpu.make_async_copy(x_any, x_ref, local_sem.at[3])
    mine[0].start()
    stream_in.start()
    mine[1].start()
    mine[2].start()

    barrier = pltpu.get_barrier_semaphore()
    for target in (beside, across, twin):
        pl.semaphore_signal(barrier, inc=1, device_id=target, device_id_type=MESH)
    for there, target in (
        (has_up, above), (has_dn, below), (has_next, (p + 1, tp)), (has_prev, (p - 1, tp)),
    ):
        @pl.when(there)
        def _():
            pl.semaphore_signal(barrier, inc=1, device_id=target, device_id_type=MESH)

    one = lambda there: jnp.where(there, 1, 0)
    pl.semaphore_wait(barrier, 3 + one(has_up) + one(has_dn) + one(has_next) + one(has_prev))

    def start_own(kind):
        for i in range(z_pieces(kind)):
            @pl.when(has_up)
            def _():
                z_copy(kind, z, i, True).start()

            @pl.when(has_dn)
            def _():
                z_copy(kind, z, i, False).start()

    mine[0].wait()
    start_own(0)
    mine[1].wait()
    start_own(1)
    stream_in.wait()

    @pl.when(has_next)
    def _():
        halo_copy().start()

    d_copy(0, z, c).start()
    d_copy(1, z, c).start()
    mine[2].wait()
    for slot in range(4):
        p_copy(z, slot, c).start()

    @pl.when(has_up & (z == 0))
    def _():
        for i in range(2):
            z_copy(2, z, i, True).start()

    @pl.when(has_dn & (z == nz - 1))
    def _():
        for i in range(2):
            z_copy(2, z, i, False).start()

    def each(t, body):
        for sign in (-1, 1):
            src = z + sign * t

            @pl.when((src >= 0) & (src < nz))
            def _():
                body(src, sign)

    def pass_on(kind, src, sign, i):
        z_copy(kind, src, i, True).wait_recv()
        if sign < 0:
            @pl.when(has_up)
            def _():
                z_copy(kind, src, i, True).start()
        else:
            @pl.when(has_dn)
            def _():
                z_copy(kind, src, i, False).start()

    def relay(kind):
        def body(src, sign):
            pass_on(kind, src, sign, 0)
            x_copy(kind, src, 0, False).start()
            y_copy(kind, src, 0, False).start()
            d_piece(kind, src, q * quarter, quarter).start()

        return body

    def onward(i):
        def body(src, sign):
            pass_on(2, src, sign, i)
            p_copy(src, i, c).start()

        return body

    def sideways(i):
        def body(src, sign):
            @pl.when(i == 0)
            def _():
                x_copy(2, src, 0, False).start()

            @pl.when(i == 1)
            def _():
                y_copy(2, src, 0, False).start()

        return body

    def diagonal(kind):
        def body(src, sign):
            x_copy(kind, src, 0, True).wait_recv()
            y_copy(kind, src, 1, False).start()
            d_piece(kind, src, qx * quarter, quarter).start()
            y_copy(kind, src, 0, True).wait_recv()
            x_copy(kind, src, 1, False).start()
            d_piece(kind, src, qy * quarter, quarter).start()

        return body

    def finish(kind):
        def body(src, sign):
            x_copy(kind, src, 1, True).wait_recv()
            d_piece(kind, src, qd * quarter, half).start()
            y_copy(kind, src, 1, True).wait_recv()
            d_piece(kind, src, qd * quarter + half, half).start()

        return body

    def arrived(src, sign):
        x_copy(2, src, 0, True).wait_recv()
        p_copy(src, 2, c).start()
        y_copy(2, src, 0, True).wait_recv()
        p_copy(src, 3, c).start()

    def norm_into(ref, base, count):
        @pl.loop(0, count // 16)
        def _(r):
            full = ref[pl.ds(pl.multiple_of(r * 16, 16), 16), :].astype(F32)
            scale = lax.rsqrt(jnp.mean(full * full, axis=1, keepdims=True) + EPS)
            normed[pl.ds(pl.multiple_of(base + r * 16, 16), 16), :] = (full * scale * gain_ref[...]).astype(BF16)

    norm_into(x_ref, HALO, rows)
    for i in range(nz):
        taps[i, 0:kw] = taps_ref[:, i * block:(i + 1) * block].astype(F32)
        taps[i, kw:kw + 1] = bias_ref[:, i * block:(i + 1) * block]

    @pl.when(has_prev)
    def _():
        halo_copy().wait_recv()

    @pl.when(jnp.logical_not(has_prev))
    def _():
        xh[...] = jnp.zeros_like(xh)

    norm_into(xh, 0, HALO)

    tile = 64
    lead = HALO - (kw - 1)
    nt = (((1,), (1,)), ((), ()))

    def on_planes(t, body):
        def one_side(side, carry):
            src = z + (2 * side - 1) * t
            valid = (src >= 0) & (src < nz) & ((t > 0) | (side == 0))

            @pl.when(valid)
            def _():
                body(side, src)

            return carry

        lax.fori_loop(0, 2, one_side, 0)

    def gate(t):
        def body(side, src):
            d_copy(0, src, 1 - c).wait_recv()
            d_copy(1, src, 1 - c).wait_recv()
            linear = lax.dot_general(normed[...], held[0, src], nt, preferred_element_type=F32)
            gating = lax.dot_general(normed[...], held[1, src], nt, preferred_element_type=F32)
            mixed = (linear * jax.nn.sigmoid(gating)).astype(BF16).astype(F32)
            for s in range(strips):
                mix[side, s, 0:HALO + rows] = mixed[:, s * lanes:(s + 1) * lanes]

        on_planes(t, body)

    def convolve(t):
        def body(side, src):
            @pl.loop(0, rows // tile)
            def _(r):
                base = pl.multiple_of(r * tile, tile)
                for s in range(strips):
                    lane = slice(s * lanes, (s + 1) * lanes)
                    total = jnp.broadcast_to(taps[src, kw:kw + 1, lane], (tile, lanes))
                    for b in range(8):
                        slab = mix[side, s, pl.ds(base + b, tile + HALO), :]
                        for a in range(HALO // 8 + 1):
                            tap = 8 * a + b - lead
                            if 0 <= tap < kw:
                                total = total + taps[src, tap:tap + 1, lane] * slab[8 * a:8 * a + tile]
                    conv[src, pl.ds(base, tile), lane] = total

        on_planes(t, body)

    slots = 2 * (nz - 1)

    @pl.loop(0, slots)
    def _(m):
        each(1 + m // 2, relay(m % 2))

        @pl.when((m % 2 == 1) & (1 + m // 2 == z) & has_up)
        def _():
            for i in range(2):
                z_copy(2, z, i, True).start()

        @pl.when((m % 2 == 1) & (1 + m // 2 == nz - 1 - z) & has_dn)
        def _():
            for i in range(2):
                z_copy(2, z, i, False).start()

        @pl.when(m >= 2)
        def _():
            each(m // 2, diagonal(m % 2))

        @pl.when(m == 0)
        def _():
            gate(0)

        @pl.when(m == 1)
        def _():
            convolve(0)

    @pl.loop(0, slots)
    def _(m):
        t, i = 1 + m // 2, m % 2
        each(t, onward(i))

        @pl.when(m < 2)
        def _():
            each(nz - 1, diagonal(i))

        @pl.when(m == 1)
        def _():
            each(1, sideways(0))
            each(1, sideways(1))

        @pl.when(m >= 2)
        def _():
            each(t, sideways(i))

        @pl.when(i == 0)
        def _():
            @pl.when(m > 0)
            def _():
                convolve(t - 1)

            each(t, finish(0))
            each(t, finish(1))

        @pl.when(i == 1)
        def _():
            gate(t)

    convolve(nz - 1)

    channels = nz * block

    @pl.loop(0, rows // 16)
    def _(r):
        here = pl.ds(pl.multiple_of(r * 16, 16), 16)
        parts = [conv[i, here, :] for i in range(nz)]
        mean = sum(jnp.sum(v, axis=1, keepdims=True) for v in parts) / channels
        meansq = sum(jnp.sum(v * v, axis=1, keepdims=True) for v in parts) / channels
        scale = lax.rsqrt(meansq - mean * mean + EPS)
        for i, v in enumerate(parts):
            lane = slice(i * block, (i + 1) * block)
            u = (v - mean) * scale * lng_ref[:, lane] + lnb_ref[:, lane]
            act[i, here, :] = (u * jax.nn.sigmoid(u)).astype(BF16)

    def out_copy(n):
        here = cols(p_cols(n), quarter)
        return pltpu.make_async_copy(out_ref.at[:, here], out_any.at[:, here], out_sem.at[n])

    @pl.loop(0, 4)
    def _(n):
        @pl.when(n == 2)
        def _():
            @pl.loop(1, nz)
            def _(t):
                each(t, arrived)

        @pl.loop(0, nz)
        def _(src):
            p_copy(src, n, 1 - c).wait_recv()

        here = cols(p_cols(n), quarter)
        total = x_ref[:, here].astype(F32)
        for i in range(nz):
            total = total + jnp.dot(act[i], held[2, i, :, here], preferred_element_type=F32)
        out_ref[:, here] = total.astype(BF16)
        out_copy(n).start()

    for n in range(4):
        out_copy(n).wait()

    @pl.when(has_next)
    def _():
        halo_copy().wait_send()

    for kind in range(3):
        @pl.loop(0, nz)
        def _(src):
            if final(kind):
                for slot in range(4):
                    p_copy(src, slot, c).wait_send()
            else:
                d_copy(kind, src, c).wait_send()

            @pl.when(src != z)
            def _():
                for i in range(2 if kind < 2 else 1):
                    x_copy(kind, src, i, False).wait_send()
                    y_copy(kind, src, i, False).wait_send()

            for i in range(z_pieces(kind)):
                @pl.when((src <= z) & has_up)
                def _():
                    z_copy(kind, src, i, True).wait_send()

                @pl.when((src >= z) & has_dn)
                def _():
                    z_copy(kind, src, i, False).wait_send()


def local(nsp, ntp, stream, norm_gain, w_lin, w_gate, conv_taps, conv_bias, ln_gain, ln_shift, w_proj):
    _, rows, width = stream.shape
    kw, channels = conv_taps.shape
    nz = ntp // 2
    block = channels // nz
    lanes = min(128, block)
    vmem = pl.BlockSpec(memory_space=pltpu.VMEM)
    anyw = pl.BlockSpec(memory_space=pl.ANY)
    dma = pltpu.SemaphoreType.DMA
    out = pl.pallas_call(
        functools.partial(kernel, nsp, nz, kw),
        out_shape=jax.ShapeDtypeStruct((rows, width), BF16),
        in_specs=[anyw, vmem, anyw, anyw, anyw, vmem, vmem, vmem, vmem],
        out_specs=anyw,
        scratch_shapes=[
            pltpu.VMEM((rows, width), BF16),
            pltpu.VMEM((rows, width), BF16),
            pltpu.VMEM((3, nz, block, width), BF16),
            pltpu.VMEM((HALO, width), BF16),
            pltpu.VMEM((HALO + rows, width), BF16),
            pltpu.VMEM((2, block // lanes, HALO + rows + 8, lanes), F32),
            pltpu.VMEM((nz, rows, block), F32),
            pltpu.VMEM((nz, rows, block), BF16),
            pltpu.VMEM((nz, kw + 1, block), F32),
            dma((4,)), dma((4,)), dma((2,)),
            dma((3, nz, 2)), dma((3, nz, 2)), dma((3, nz, 2)), dma((3, nz)),
            dma((3, nz, 2)), dma((3, nz, 2)), dma((3, nz, 2)), dma((3, nz, 2)), dma((3, nz)), dma((nz, 4)), dma((nz, 4)),
        ],
        compiler_params=pltpu.CompilerParams(
            collective_id=0, has_side_effects=True, vmem_limit_bytes=32 * 1024 * 1024
        ),
    )(
        stream[0], norm_gain[None], w_lin, w_gate, w_proj, conv_taps,
        conv_bias[None], ln_gain[None], ln_shift[None],
    )
    return out[None]


def solution(mesh):
    placed = (
        P("tp", "sp", None), P(), P("tp", None), P("tp", None), P(), P(), P(), P(), P("tp", None),
    )
    return jax.shard_map(
        functools.partial(local, mesh.shape["sp"], mesh.shape["tp"]),
        mesh=mesh, in_specs=placed, out_specs=P("tp", "sp", None), check_vma=False,
    )
```

```python
import functools

import jax
import jax.numpy as jnp
from jax import lax
from jax.experimental import pallas as pl
from jax.experimental.pallas import tpu as pltpu
from jax.sharding import PartitionSpec as P

EPS = 1e-06
HALO = 32
F32 = jnp.float32
BF16 = jnp.bfloat16
MESH = pl.DeviceIdType.MESH


def kernel(
    nsp, nz, kw,
    x_any, gain_any, wl_ref, wg_ref, wp_ref, taps_any, bias_any, lng_any, lnb_any,
    out_any,
    x_ref, out_ref, gain_ref, taps_ref, bias_ref, lng_ref, lnb_ref, held, xh, normed, mix, conv, act, taps,
    local_sem, out_sem, halo_sem, z_recv, x_recv, y_recv, d_recv, up_send, dn_send, x_send, y_send, d_send, dp_recv, dp_send,
):
    rows, width = x_ref.shape
    block = held.shape[2]
    shard = block // 2
    lanes = min(128, block)
    strips = block // lanes
    quarter = width // 4
    half = quarter // 2
    p, tp = lax.axis_index("sp"), lax.axis_index("tp")
    z, c = tp // 2, tp % 2
    q = p % 4
    low, high = q % 2, q // 2
    beside = (p + 1 - 2 * low, tp)
    across = (p + 2 - 4 * high, tp)
    twin = (p, z * 2 + 1 - c)
    above = (p, tp + 2)
    below = (p, tp - 2)
    parity = (low + high) % 2
    has_up, has_dn = z < nz - 1, z > 0
    has_next, has_prev = p < nsp - 1, p > 0
    qx, qy, qd = q + 1 - 2 * low, q + 2 - 4 * high, 3 - q

    def cols(start, size):
        return pl.ds(pl.multiple_of(start, 128), size)

    def at(kind, src, core, start, size):
        return held.at[kind, src, pl.ds(pl.multiple_of(core * shard, 16), shard), cols(start, size)]

    def send(piece, ssem, rsem, target):
        return pltpu.make_async_remote_copy(
            src_ref=piece, dst_ref=piece, send_sem=ssem, recv_sem=rsem, device_id=target, device_id_type=MESH
        )

    def final(kind):
        return isinstance(kind, int) and kind == 2

    def z_piece(kind, src, i):
        if not final(kind):
            return at(kind, src, c, q * quarter, quarter)
        return at(kind, src, c, (parity * 2 + i) * quarter, quarter)

    def z_copy(kind, src, i, up):
        return send(
            z_piece(kind, src, i), (up_send if up else dn_send).at[kind, src, i], z_recv.at[kind, src, i],
            above if up else below,
        )

    def z_pieces(kind):
        return 2 if final(kind) else 1

    def x_copy(kind, src, i, incoming):
        if final(kind):
            piece = at(2, src, c, ((1 - parity if incoming else parity) * 2) * quarter, quarter)
        elif i == 0:
            piece = at(kind, src, c, (qx if incoming else q) * quarter, quarter)
        else:
            piece = at(kind, src, c, (qd if incoming else qy) * quarter, half)
        return send(piece, x_send.at[kind, src, i], x_recv.at[kind, src, i], beside)

    def y_copy(kind, src, i, incoming):
        if final(kind):
            piece = at(2, src, c, ((1 - parity if incoming else parity) * 2 + 1) * quarter, quarter)
        elif i == 0:
            piece = at(kind, src, c, (qy if incoming else q) * quarter, quarter)
        else:
            piece = at(kind, src, c, (qd if incoming else qx) * quarter + half, half)
        return send(piece, y_send.at[kind, src, i], y_recv.at[kind, src, i], across)

    def d_copy(kind, src, core):
        return send(at(kind, src, core, 0, width), d_send.at[kind, src], d_recv.at[kind, src], twin)

    def d_piece(kind, src, start, size):
        return send(at(kind, src, c, start, size), d_send.at[kind, src], d_recv.at[kind, src], twin)

    def p_cols(slot):
        return ((parity + slot // 2) % 2 * 2 + slot % 2) * quarter

    def p_copy(src, slot, core):
        return send(at(2, src, core, p_cols(slot), quarter), dp_send.at[src, slot], dp_recv.at[src, slot], twin)

    def halo_copy():
        return pltpu.make_async_remote_copy(
            src_ref=x_ref.at[pl.ds(rows - HALO, HALO)], dst_ref=xh, send_sem=halo_sem.at[0],
            recv_sem=halo_sem.at[1], device_id=(p + 1, tp), device_id_type=MESH,
        )

    mine = [
        pltpu.make_async_copy(ref, at(kind, z, c, 0, width), local_sem.at[kind])
        for kind, ref in enumerate((wl_ref, wg_ref, wp_ref))
    ]
    stream_in = pltpu.make_async_copy(x_any, x_ref, local_sem.at[3])
    mine[0].start()
    stream_in.start()
    mine[1].start()
    small = [
        pltpu.make_async_copy(ref, there, local_sem.at[4 + i])
        for i, (ref, there) in enumerate((
            (gain_any, gain_ref), (taps_any, taps_ref), (bias_any, bias_ref), (lng_any, lng_ref), (lnb_any, lnb_ref),
        ))
    ]
    for copy in small:
        copy.start()
    mine[2].start()

    barrier = pltpu.get_barrier_semaphore()
    for target in (beside, across, twin):
        pl.semaphore_signal(barrier, inc=1, device_id=target, device_id_type=MESH)
    for there, target in (
        (has_up, above), (has_dn, below), (has_next, (p + 1, tp)), (has_prev, (p - 1, tp)),
    ):
        @pl.when(there)
        def _():
            pl.semaphore_signal(barrier, inc=1, device_id=target, device_id_type=MESH)

    one = lambda there: jnp.where(there, 1, 0)
    pl.semaphore_wait(barrier, 3 + one(has_up) + one(has_dn) + one(has_next) + one(has_prev))

    def start_own(kind):
        for i in range(z_pieces(kind)):
            @pl.when(has_up)
            def _():
                z_copy(kind, z, i, True).start()

            @pl.when(has_dn)
            def _():
                z_copy(kind, z, i, False).start()

    mine[0].wait()
    start_own(0)
    mine[1].wait()
    start_own(1)
    stream_in.wait()

    @pl.when(has_next)
    def _():
        halo_copy().start()

    d_copy(0, z, c).start()
    d_copy(1, z, c).start()
    mine[2].wait()
    for slot in range(4):
        p_copy(z, slot, c).start()

    @pl.when(has_up & (z == 0))
    def _():
        for i in range(2):
            z_copy(2, z, i, True).start()

    @pl.when(has_dn & (z == nz - 1))
    def _():
        for i in range(2):
            z_copy(2, z, i, False).start()

    def each(t, body):
        for sign in (-1, 1):
            src = z + sign * t

            @pl.when((src >= 0) & (src < nz))
            def _():
                body(src, sign)

    def pass_on(kind, src, sign, i):
        z_copy(kind, src, i, True).wait_recv()
        if sign < 0:
            @pl.when(has_up)
            def _():
                z_copy(kind, src, i, True).start()
        else:
            @pl.when(has_dn)
            def _():
                z_copy(kind, src, i, False).start()

    def relay(kind):
        def body(src, sign):
            pass_on(kind, src, sign, 0)
            x_copy(kind, src, 0, False).start()
            y_copy(kind, src, 0, False).start()
            d_piece(kind, src, q * quarter, quarter).start()

        return body

    def onward(i):
        def body(src, sign):
            pass_on(2, src, sign, i)
            p_copy(src, i, c).start()

        return body

    def sideways(i):
        def body(src, sign):
            @pl.when(i == 0)
            def _():
                x_copy(2, src, 0, False).start()

            @pl.when(i == 1)
            def _():
                y_copy(2, src, 0, False).start()

        return body

    def diagonal(kind):
        def body(src, sign):
            x_copy(kind, src, 0, True).wait_recv()
            y_copy(kind, src, 1, False).start()
            d_piece(kind, src, qx * quarter, quarter).start()
            y_copy(kind, src, 0, True).wait_recv()
            x_copy(kind, src, 1, False).start()
            d_piece(kind, src, qy * quarter, quarter).start()

        return body

    def finish(kind):
        def body(src, sign):
            x_copy(kind, src, 1, True).wait_recv()
            d_piece(kind, src, qd * quarter, half).start()
            y_copy(kind, src, 1, True).wait_recv()
            d_piece(kind, src, qd * quarter + half, half).start()

        return body

    def arrived(src, sign):
        x_copy(2, src, 0, True).wait_recv()
        p_copy(src, 2, c).start()
        y_copy(2, src, 0, True).wait_recv()
        p_copy(src, 3, c).start()

    def norm_into(ref, base, count):
        @pl.loop(0, count // 16)
        def _(r):
            full = ref[pl.ds(pl.multiple_of(r * 16, 16), 16), :].astype(F32)
            scale = lax.rsqrt(jnp.mean(full * full, axis=1, keepdims=True) + EPS)
            normed[pl.ds(pl.multiple_of(base + r * 16, 16), 16), :] = (full * scale * gain_ref[...]).astype(BF16)

    for copy in small:
        copy.wait()
    norm_into(x_ref, HALO, rows)
    for i in range(nz):
        taps[i, 0:kw] = taps_ref[:, i * block:(i + 1) * block].astype(F32)
        taps[i, kw:kw + 1] = bias_ref[:, i * block:(i + 1) * block]

    @pl.when(has_prev)
    def _():
        halo_copy().wait_recv()

    @pl.when(jnp.logical_not(has_prev))
    def _():
        xh[...] = jnp.zeros_like(xh)

    norm_into(xh, 0, HALO)

    tile = 64
    lead = HALO - (kw - 1)
    nt = (((1,), (1,)), ((), ()))

    def on_planes(t, body):
        def one_side(side, carry):
            src = z + (2 * side - 1) * t
            valid = (src >= 0) & (src < nz) & ((t > 0) | (side == 0))

            @pl.when(valid)
            def _():
                body(side, src)

            return carry

        lax.fori_loop(0, 2, one_side, 0)

    def gate(t):
        def body(side, src):
            d_copy(0, src, 1 - c).wait_recv()
            d_copy(1, src, 1 - c).wait_recv()
            linear = lax.dot_general(normed[...], held[0, src], nt, preferred_element_type=F32)
            gating = lax.dot_general(normed[...], held[1, src], nt, preferred_element_type=F32)
            mixed = (linear * jax.nn.sigmoid(gating)).astype(BF16).astype(F32)
            for s in range(strips):
                mix[side, s, 0:HALO + rows] = mixed[:, s * lanes:(s + 1) * lanes]

        on_planes(t, body)

    def convolve(t):
        def body(side, src):
            @pl.loop(0, rows // tile)
            def _(r):
                base = pl.multiple_of(r * tile, tile)
                for s in range(strips):
                    lane = slice(s * lanes, (s + 1) * lanes)
                    total = jnp.broadcast_to(taps[src, kw:kw + 1, lane], (tile, lanes))
                    for b in range(8):
                        slab = mix[side, s, pl.ds(base + b, tile + HALO), :]
                        for a in range(HALO // 8 + 1):
                            tap = 8 * a + b - lead
                            if 0 <= tap < kw:
                                total = total + taps[src, tap:tap + 1, lane] * slab[8 * a:8 * a + tile]
                    conv[src, pl.ds(base, tile), lane] = total

        on_planes(t, body)

    slots = 2 * (nz - 1)

    @pl.loop(0, slots)
    def _(m):
        each(1 + m // 2, relay(m % 2))

        @pl.when((m % 2 == 1) & (1 + m // 2 == z) & has_up)
        def _():
            for i in range(2):
                z_copy(2, z, i, True).start()

        @pl.when((m % 2 == 1) & (1 + m // 2 == nz - 1 - z) & has_dn)
        def _():
            for i in range(2):
                z_copy(2, z, i, False).start()

        @pl.when(m >= 2)
        def _():
            each(m // 2, diagonal(m % 2))

        @pl.when(m == 0)
        def _():
            gate(0)

        @pl.when(m == 1)
        def _():
            convolve(0)

    @pl.loop(0, slots)
    def _(m):
        t, i = 1 + m // 2, m % 2
        each(t, onward(i))

        @pl.when(m < 2)
        def _():
            each(nz - 1, diagonal(i))

        @pl.when(m == 1)
        def _():
            each(1, sideways(0))
            each(1, sideways(1))

        @pl.when(m >= 2)
        def _():
            each(t, sideways(i))

        @pl.when(i == 0)
        def _():
            @pl.when(m > 0)
            def _():
                convolve(t - 1)

            each(t, finish(0))
            each(t, finish(1))

        @pl.when(i == 1)
        def _():
            gate(t)

    convolve(nz - 1)

    channels = nz * block

    @pl.loop(0, rows // 16)
    def _(r):
        here = pl.ds(pl.multiple_of(r * 16, 16), 16)
        parts = [conv[i, here, :] for i in range(nz)]
        mean = sum(jnp.sum(v, axis=1, keepdims=True) for v in parts) / channels
        meansq = sum(jnp.sum(v * v, axis=1, keepdims=True) for v in parts) / channels
        scale = lax.rsqrt(meansq - mean * mean + EPS)
        for i, v in enumerate(parts):
            lane = slice(i * block, (i + 1) * block)
            u = (v - mean) * scale * lng_ref[:, lane] + lnb_ref[:, lane]
            act[i, here, :] = (u * jax.nn.sigmoid(u)).astype(BF16)

    def out_copy(n):
        here = cols(p_cols(n), quarter)
        return pltpu.make_async_copy(out_ref.at[:, here], out_any.at[:, here], out_sem.at[n])

    @pl.loop(0, 4)
    def _(n):
        @pl.when(n == 2)
        def _():
            @pl.loop(1, nz)
            def _(t):
                each(t, arrived)

        @pl.loop(0, nz)
        def _(src):
            p_copy(src, n, 1 - c).wait_recv()

        here = cols(p_cols(n), quarter)
        total = x_ref[:, here].astype(F32)
        for i in range(nz):
            total = total + jnp.dot(act[i], held[2, i, :, here], preferred_element_type=F32)
        out_ref[:, here] = total.astype(BF16)
        out_copy(n).start()

    for n in range(4):
        out_copy(n).wait()

    @pl.when(has_next)
    def _():
        halo_copy().wait_send()

    for kind in range(3):
        @pl.loop(0, nz)
        def _(src):
            if final(kind):
                for slot in range(4):
                    p_copy(src, slot, c).wait_send()
            else:
                d_copy(kind, src, c).wait_send()

            @pl.when(src != z)
            def _():
                for i in range(2 if kind < 2 else 1):
                    x_copy(kind, src, i, False).wait_send()
                    y_copy(kind, src, i, False).wait_send()

            for i in range(z_pieces(kind)):
                @pl.when((src <= z) & has_up)
                def _():
                    z_copy(kind, src, i, True).wait_send()

                @pl.when((src >= z) & has_dn)
                def _():
                    z_copy(kind, src, i, False).wait_send()


def local(nsp, ntp, stream, norm_gain, w_lin, w_gate, conv_taps, conv_bias, ln_gain, ln_shift, w_proj):
    _, rows, width = stream.shape
    kw, channels = conv_taps.shape
    nz = ntp // 2
    block = channels // nz
    lanes = min(128, block)
    kept = pl.BlockSpec(memory_space=pltpu.HBM)
    dma = pltpu.SemaphoreType.DMA
    out = pl.pallas_call(
        functools.partial(kernel, nsp, nz, kw),
        out_shape=jax.ShapeDtypeStruct((rows, width), BF16),
        in_specs=[kept] * 9,
        out_specs=pl.BlockSpec(memory_space=pl.ANY),
        scratch_shapes=[
            pltpu.VMEM((rows, width), BF16),
            pltpu.VMEM((rows, width), BF16),
            pltpu.VMEM((1, width), F32),
            pltpu.VMEM((kw, channels), BF16),
            pltpu.VMEM((1, channels), F32),
            pltpu.VMEM((1, channels), F32),
            pltpu.VMEM((1, channels), F32),
            pltpu.VMEM((3, nz, block, width), BF16),
            pltpu.VMEM((HALO, width), BF16),
            pltpu.VMEM((HALO + rows, width), BF16),
            pltpu.VMEM((2, block // lanes, HALO + rows + 8, lanes), F32),
            pltpu.VMEM((nz, rows, block), F32),
            pltpu.VMEM((nz, rows, block), BF16),
            pltpu.VMEM((nz, kw + 1, block), F32),
            dma((9,)), dma((4,)), dma((2,)),
            dma((3, nz, 2)), dma((3, nz, 2)), dma((3, nz, 2)), dma((3, nz)),
            dma((3, nz, 2)), dma((3, nz, 2)), dma((3, nz, 2)), dma((3, nz, 2)), dma((3, nz)), dma((nz, 4)), dma((nz, 4)),
        ],
        compiler_params=pltpu.CompilerParams(
            collective_id=0, has_side_effects=True, vmem_limit_bytes=60 * 1024 * 1024
        ),
    )(
        stream[0], norm_gain[None], w_lin, w_gate, w_proj, conv_taps,
        conv_bias[None], ln_gain[None], ln_shift[None],
    )
    return out[None]


def solution(mesh):
    placed = (
        P("tp", "sp", None), P(), P("tp", None), P("tp", None), P(), P(), P(), P(), P("tp", None),
    )
    return jax.shard_map(
        functools.partial(local, mesh.shape["sp"], mesh.shape["tp"]),
        mesh=mesh, in_specs=placed, out_specs=P("tp", "sp", None), check_vma=False,
    )
```
